32 devices in a mesh: grp: 1, sp: 16 (over z, y, core), tp: 2 (over x).
Axes of the slice: x: 2, y: 2, z: 4, core: 2. Of those that a mesh axis runs over, the one named last changes fastest.
Arguments:
- residual: bfloat16 [8192, 2048], P(('grp', 'sp', 'tp')), may hold values from -6 to 6
- queries: bfloat16 [8192, 2048], P(('grp', 'sp'), 'tp'), may hold values from -200 to 200
- key_heads: bfloat16 [8192, 256], P(('grp', 'sp'), 'tp'), may hold values from -8 to 8
- value_heads: bfloat16 [8192, 256], P(('grp', 'sp'), 'tp'), may hold values from -6 to 6
- documents: int32 [8192], P(('grp', 'sp')), may hold values from 0 to 3, never falling along the last dimension, each value on 1 to 4096 neighbouring positions
- sink_logits: float32 [32], P('tp'), may hold values from 4 to 7
- out_weight: bfloat16 [2048, 2048], P('tp'), may hold values from -1 to 1
- norm_gain: bfloat16 [2048], replicated, may hold values from 0.099609375 to 1.8984375
- gate_weight: bfloat16 [2048, 5632], P('sp', 'tp'), may hold values from -0.125 to 0.125
- up_weight: bfloat16 [2048, 5632], P('sp', 'tp'), may hold values from -0.125 to 0.125
- down_weight: bfloat16 [2048, 5632], P('sp', 'tp'), may hold values from -0.078125 to 0.078125
Outputs:
- updated: bfloat16 [8192, 2048], P(('grp', 'sp', 'tp'))
The draws below stay inside these ranges and needn't reach their ends.
Inputs may be any that keep to these rules, and one draw needn't show every extreme that they name: `documents`: document numbers never fall along the sequence.
All inputs are finite; a program needn't handle non-finite values.
Results may differ from the reference program's by a relative error of at most 0.012.
Values may be sent and summed in bfloat16 or wider, within the bound.
A program may use at most 128 MiB of HBM per device.

```python
import math
import jax
import jax.numpy as jnp
import numpy as np
from jax import lax

D = 2048
HD = 64
QH = 32
KVH = 4
FF = 5632
WINDOW = 128
TOK_DEV = 512
SEQ = 8192
DOCS = 4
N_TP = 2


def drawn_pair(key):
    key_first = jax.random.fold_in(key, 11)
    key_second = jax.random.fold_in(key, 12)
    keys_base = jax.random.normal(key_first, (SEQ, KVH * HD), jnp.float32)
    query_base = jax.random.normal(key_second, (SEQ, QH * HD), jnp.float32)
    keys_out = keys_base
    query_out = query_base
    return (query_out, keys_out)


def draw_queries(key, part):
    return drawn_pair(key)[0].astype(jnp.bfloat16)


def draw_key_heads(key, part):
    return drawn_pair(key)[1].astype(jnp.bfloat16)


def block_levels(key, extent, cuts, low, top_value):
    factor_of = 1.0
    for axis_at, blocks in cuts:
        steps = jax.random.uniform(jax.random.fold_in(jax.random.fold_in(key, 6), axis_at), (blocks,), jnp.float32, low / len(cuts), top_value / len(cuts))
        factor_of = factor_of * jnp.repeat(jnp.exp(steps), extent[axis_at] // blocks).reshape((-1,) + (1,) * (len(extent) - 1 - axis_at))
    return factor_of


def split_up(amount, total, reach, skew):
    portions = [(1 << 20) // math.isqrt(rank ** skew) + 1 for rank in range(2, amount + 1)]
    surplus, counts = total - reach - (amount - 1), [1] * (amount - 1)
    while surplus > 0:
        free = [i for i in range(amount - 1) if counts[i] < reach]
        mass, budget = sum([portions[i] for i in free]), surplus
        for i in free:
            addition = min(reach - counts[i], max(1, budget * portions[i] // mass), surplus)
            counts[i] = counts[i] + addition
            surplus = surplus - addition
    return np.array([reach] + counts)


def ragged_sizes(key, count, total, bound, lean):
    if count == 2:
        one = jax.random.randint(key, (), max(1, total - bound), min(bound, total - 1) + 1)
        return jnp.stack([one, total - one])
    lengths = jnp.asarray(split_up(count, total, bound, lean), jnp.int32)
    pairs = (count - 1) // 2
    donor, sink = lengths[1:1 + 2 * pairs:2], lengths[2:2 + 2 * pairs:2]
    room = jnp.minimum(donor - 1, bound - sink)
    moved = jax.random.randint(jax.random.fold_in(key, 1), (pairs,), 0, 1 << 20) % (room + 1)
    lengths = lengths.at[1:1 + 2 * pairs:2].set(donor - moved).at[2:2 + 2 * pairs:2].set(sink + moved)
    return lengths[jax.random.permutation(jax.random.fold_in(key, 2), count)]


def scatter_about(own_key, dims, scale, bound, pieces=(), kind=jnp.bfloat16):
    loudness = block_levels(own_key, dims, pieces, -0.22, 0.18) if pieces else 1.0
    entries = jax.random.normal(own_key, dims, jnp.float32) * scale * loudness
    return jnp.minimum(jnp.maximum(entries, -bound), bound).astype(kind)


def setup_inputs(seed: int = 0, part: int = 0) -> dict:
    streams_of = jax.random.split(jax.random.key(seed), 12)
    part_splits = jax.random.split(jax.random.fold_in(streams_of[11], part), 12)
    return {
        "residual": scatter_about(part_splits[0], (SEQ, D), 1.0, 6.0, ((0, 32),)),
        "queries": draw_queries(jax.random.fold_in(jax.random.fold_in(streams_of[11], part), 71), part),
        "key_heads": draw_key_heads(jax.random.fold_in(jax.random.fold_in(streams_of[11], part), 71), part),
        "value_heads": scatter_about(part_splits[3], (SEQ, KVH * HD), 1.0, 6.0, ((0, 16), (1, 2))),
        "documents": jnp.searchsorted(jnp.cumsum(ragged_sizes(part_splits[4], DOCS, SEQ, SEQ // 2, 2)), jnp.arange(SEQ), side="right").astype(jnp.int32),
        "sink_logits": jnp.clip(4.0 + 3.0 * jax.random.uniform(streams_of[5], (QH,), jnp.float32) ** block_levels(streams_of[5], (QH,), ((0, 2),), -0.2, 0.2), 4.0, 7.0),
        "out_weight": scatter_about(streams_of[6], (QH * HD, D), QH ** -0.5, 1.0, ((0, 2),)),
        "norm_gain": jnp.clip(1.0 + 0.18 * jax.random.normal(streams_of[7], (D,), jnp.float32), 0.099609375, 1.8984375).astype(jnp.bfloat16),
        "gate_weight": scatter_about(streams_of[8], (D, FF), D ** -0.5, 0.125, ((0, 16), (1, 2))),
        "up_weight": scatter_about(streams_of[9], (D, FF), D ** -0.5, 0.125, ((0, 16), (1, 2))),
        "down_weight": scatter_about(streams_of[10], (D, FF), FF ** -0.5, 0.078125, ((0, 16), (1, 2))),
    }


epsilon = 1e-06
masked = -1e+30

def reference(residual, queries, key_heads, value_heads, documents, sink_logits, out_weight, norm_gain, gate_weight, up_weight, down_weight):
    length = queries.shape[0]
    groups = QH // KVH
    blocks = length // TOK_DEV
    padded_keys = jnp.pad(key_heads, ((WINDOW, WINDOW), (0, 0)))
    padded_values = jnp.pad(value_heads, ((WINDOW, WINDOW), (0, 0)))
    padded_docs = jnp.pad(documents, (WINDOW, WINDOW))
    sink_table = sink_logits.astype(jnp.float32).reshape(KVH, groups)[:, :, None]

    def attend_block(block_index):
        row_start = (block_index * TOK_DEV).astype(jnp.int32)
        query_block = lax.dynamic_slice_in_dim(queries, row_start, TOK_DEV, 0).astype(jnp.float32).reshape(TOK_DEV, KVH, groups, HD)
        key_block = lax.dynamic_slice_in_dim(padded_keys, row_start, TOK_DEV + 2 * WINDOW, 0).astype(jnp.float32).reshape(-1, KVH, HD)
        value_block = lax.dynamic_slice_in_dim(padded_values, row_start, TOK_DEV + 2 * WINDOW, 0).astype(jnp.float32).reshape(-1, KVH, HD)
        query_docs = lax.dynamic_slice_in_dim(documents, row_start, TOK_DEV, 0)
        key_docs = lax.dynamic_slice_in_dim(padded_docs, row_start, TOK_DEV + 2 * WINDOW, 0)
        query_pos = row_start + jnp.arange(TOK_DEV, dtype=jnp.int32)
        key_pos = row_start - WINDOW + jnp.arange(TOK_DEV + 2 * WINDOW, dtype=jnp.int32)
        allowed = (jnp.abs(query_pos[:, None] - key_pos[None, :]) <= WINDOW) & (key_pos >= 0)[None, :] & (key_pos < length)[None, :] & (query_docs[:, None] == key_docs[None, :])
        scores = jnp.einsum('qkgd,jkd->kgqj', query_block, key_block) * HD ** (-0.5)
        scores = jnp.where(allowed[None, None], scores, masked)
        row_max = jnp.maximum(lax.optimization_barrier(jnp.max(scores, axis=-1)), sink_table)
        expo = jnp.exp(scores - row_max[..., None])
        total = lax.optimization_barrier(jnp.sum(expo, axis=-1)) + jnp.exp(sink_table - row_max)
        probs = (expo / total[..., None]).astype(jnp.bfloat16)
        mixed = jnp.einsum('kgqj,jkd->qkgd', probs.astype(jnp.float32), value_block)
        return mixed.reshape(TOK_DEV, QH * HD).astype(jnp.bfloat16)
    attended = lax.map(attend_block, jnp.arange(blocks, dtype=jnp.int32)).reshape(length, QH * HD)
    projected = jnp.dot(attended, out_weight, preferred_element_type=jnp.float32).astype(jnp.bfloat16)
    middle = (residual.astype(jnp.float32) + lax.optimization_barrier(projected).astype(jnp.float32)).astype(jnp.bfloat16)
    middle_wide = middle.astype(jnp.float32)
    scaled = middle_wide * lax.rsqrt(lax.optimization_barrier(jnp.mean(middle_wide * middle_wide, axis=-1, keepdims=True)) + epsilon)
    normed = (scaled * norm_gain.astype(jnp.float32)).astype(jnp.bfloat16)
    block_width = FF // N_TP

    def mix_block(block_index):
        row_start = (block_index * TOK_DEV).astype(jnp.int32)
        row_block = lax.dynamic_slice_in_dim(normed, row_start, TOK_DEV, 0)
        gate_value = jnp.dot(row_block, gate_weight, preferred_element_type=jnp.float32)
        up_value = jnp.dot(row_block, up_weight, preferred_element_type=jnp.float32)
        hidden = (jax.nn.silu(gate_value) * up_value).astype(jnp.bfloat16)
        summed = jnp.zeros((TOK_DEV, D), jnp.float32)
        for shard_index in range(N_TP):
            columns = hidden[:, shard_index * block_width:(shard_index + 1) * block_width]
            down_block = down_weight[:, shard_index * block_width:(shard_index + 1) * block_width]
            term = lax.dot_general(columns, down_block, (((1,), (1,)), ((), ())), preferred_element_type=jnp.float32).astype(jnp.bfloat16)
            summed = summed + lax.optimization_barrier(term).astype(jnp.float32)
        return summed.astype(jnp.bfloat16)
    mixer_out = lax.map(mix_block, jnp.arange(blocks, dtype=jnp.int32)).reshape(length, D)
    updated = middle.astype(jnp.float32) + 0.5 * lax.optimization_barrier(mixer_out).astype(jnp.float32)
    return updated.astype(jnp.bfloat16)
```

```python
import jax
import jax.numpy as jnp
from jax import lax
from jax.sharding import PartitionSpec as P

HD = 64
WINDOW = 128


epsilon = 1e-06
masked = -1e30


def on_device(
    residual,
    queries,
    key_heads,
    value_heads,
    documents,
    sink_logits,
    out_weight,
    norm_gain,
    gate_weight,
    up_weight,
    down_weight,
):
    n_sp, n_tp = lax.axis_size("sp"), lax.axis_size("tp")
    width = gate_weight.shape[1]
    cores = 2 if n_sp % 2 == 0 else 1
    pair = 2 if n_sp % (2 * cores) == 0 and width % 256 == 0 else 1
    chain = n_sp // (pair * cores)
    part = width // pair
    depth = gate_weight.shape[0]
    sp, tp = lax.axis_index("sp"), lax.axis_index("tp")
    core, y, z = sp % cores, (sp // cores) % pair, sp // (cores * pair)

    def place(zi, yi, ci):
        return (zi * pair + yi) * cores + ci

    def along(array, route):
        pairs = []
        for zi in range(chain):
            for yi in range(pair):
                for ci in range(cores):
                    to = route(zi, yi, ci)
                    if to is not None:
                        pairs.append((place(zi, yi, ci), place(*to)))
        return lax.ppermute(array, "sp", pairs)

    def spread(item):
        if chain == 4:
            two = along(item, lambda a, b, c: ((a + 2) % 4, b, c))
            right = along(item, lambda a, b, c: (a + 1, b, c) if a < 3 else None)
            left = along(item, lambda a, b, c: (a - 1, b, c) if a > 0 else None)
            ends = along(two, lambda a, b, c: {1: (0, b, c), 2: (3, b, c)}.get(a))
            return [
                item,
                jnp.where(z == 3, ends, left),
                two,
                jnp.where(z == 0, ends, right),
            ]
        pieces = [item]
        for _ in range(chain - 1):
            pieces.append(along(pieces[-1], lambda a, b, c: ((a - 1) % chain, b, c)))
        return pieces

    def by_core(piece):
        if cores == 1:
            return [piece]
        return [piece, along(piece, lambda a, b, c: (a, b, 1 - c))]

    def split_pair(shard):
        mine = lax.dynamic_slice_in_dim(shard, y * part, part, axis=1)
        if pair == 1:
            return mine, None
        return mine, lax.dynamic_slice_in_dim(shard, (1 - y) * part, part, axis=1)

    def in_order(mine, other):
        if pair == 1:
            return mine
        return jnp.where(
            y == 0,
            jnp.concatenate([mine, other], axis=0),
            jnp.concatenate([other, mine], axis=0),
        )

    def swap(array):
        return along(array, lambda a, b, c: (a, 1 - b, c))

    gate_mine, gate_other = split_pair(gate_weight)
    up_mine, up_other = split_pair(up_weight)
    down_mine, down_other = split_pair(down_weight)
    joint = jnp.concatenate([gate_mine, up_mine], axis=1)
    if pair == 1:
        joint_item, down_far = joint, None
    else:
        joint_item = in_order(joint, swap(jnp.concatenate([gate_other, up_other], axis=1)))
        down_far = swap(down_other)
    joint_pieces = [by_core(piece) for piece in spread(joint_item)]
    down_pieces = spread(down_mine)
    if pair == 2:
        far_pieces = spread(down_far)
        down_pieces = [in_order(a, b) for a, b in zip(down_pieces, far_pieces)]
    down_pieces = [by_core(piece) for piece in down_pieces]

    tok_rows = queries.shape[0]
    kv_local = key_heads.shape[1] // HD
    q_local = queries.shape[1] // HD
    groups = q_local // kv_local
    own_docs = documents.astype(jnp.bfloat16)
    kv_width = key_heads.shape[1]
    travel = jnp.concatenate(
        [key_heads, value_heads, jnp.broadcast_to(own_docs[:, None], (tok_rows, 128))], axis=1
    )
    up_pairs = [(i, i + 1) for i in range(n_sp - 1)]
    before = lax.ppermute(travel[tok_rows - WINDOW :], "sp", up_pairs)
    after = lax.ppermute(travel[:WINDOW], "sp", [(j, i) for i, j in up_pairs])
    spread_all = jnp.concatenate([before, travel, after], axis=0)
    spread_keys = spread_all[:, :kv_width]
    spread_values = spread_all[:, kv_width : 2 * kv_width]
    spread_docs = spread_all[:, 2 * kv_width]
    offset = lax.axis_index("sp") * tok_rows
    total_length = tok_rows * lax.axis_size("sp")
    query_pos = offset + jnp.arange(tok_rows, dtype=jnp.int32)
    key_pos = offset - WINDOW + jnp.arange(tok_rows + 2 * WINDOW, dtype=jnp.int32)
    allowed = (
        (jnp.abs(query_pos[:, None] - key_pos[None, :]) <= WINDOW)
        & (key_pos >= 0)[None, :]
        & (key_pos < total_length)[None, :]
        & (own_docs[:, None] == spread_docs[None, :])
    )
    query_block = queries.reshape(tok_rows, kv_local, groups, HD)
    key_block = spread_keys.reshape(-1, kv_local, HD)
    value_block = spread_values.reshape(-1, kv_local, HD)
    scores = jnp.einsum(
        "qkgd,jkd->kgqj", query_block, key_block, preferred_element_type=jnp.float32
    ) * HD ** (-0.5)
    scores = jnp.where(allowed[None, None], scores, masked)
    sink_table = sink_logits.reshape(kv_local, groups)[:, :, None]
    row_max = jnp.maximum(jnp.max(scores, axis=-1), sink_table)
    expo = jnp.exp(scores - row_max[..., None])
    total = jnp.sum(expo, axis=-1) + jnp.exp(sink_table - row_max)
    probs = (expo / total[..., None]).astype(jnp.bfloat16)
    mixed = jnp.einsum("kgqj,jkd->qkgd", probs, value_block, preferred_element_type=jnp.float32)
    attended = mixed.reshape(tok_rows, q_local * HD).astype(jnp.bfloat16)
    rows = tok_rows // n_tp

    def projection(owner):
        block = lax.dynamic_slice_in_dim(attended, owner * rows, rows, axis=0)
        return jnp.dot(block, out_weight, preferred_element_type=jnp.float32)

    arrived = [
        lax.ppermute(
            projection((tp + k) % n_tp).astype(jnp.bfloat16),
            "tp",
            [(i, (i + k) % n_tp) for i in range(n_tp)],
        )
        for k in range(1, n_tp)
    ]
    total_proj = projection(tp)
    for block in arrived:
        total_proj = total_proj + block.astype(jnp.float32)
    projected = total_proj.astype(jnp.bfloat16)
    middle = (residual.astype(jnp.float32) + projected.astype(jnp.float32)).astype(jnp.bfloat16)
    middle_wide = middle.astype(jnp.float32)
    scaled = middle_wide * lax.rsqrt(
        jnp.mean(middle_wide * middle_wide, axis=-1, keepdims=True) + epsilon
    )
    normed = (scaled * norm_gain.astype(jnp.float32)).astype(jnp.bfloat16)

    near = [0, 2] if chain == 4 else list(range(chain // 2))
    order = near + [d for d in range(chain) if d not in near]
    blocks = []
    for d in order:
        for e in range(cores):
            for b in range(pair):
                at = place((z + d) % chain, b, (core + e) % cores) * depth
                blocks.append(lax.dynamic_slice_in_dim(normed, at, depth, axis=1))
    shuffled = jnp.concatenate(blocks, axis=1)

    def group_move(array, dy, dt):
        pairs = []
        for zi in range(chain):
            for yi in range(pair):
                for ci in range(cores):
                    for ti in range(n_tp):
                        to = place(zi, (yi + dy) % pair, ci) * n_tp + (ti + dt) % n_tp
                        pairs.append((place(zi, yi, ci) * n_tp + ti, to))
        return lax.ppermute(array, ("sp", "tp"), pairs)

    members = [(dy, dt) for dy in range(pair) for dt in range(n_tp)]
    row_piece = jnp.concatenate(
        [shuffled] + [group_move(shuffled, -dy, -dt) for dy, dt in members[1:]], axis=0
    )
    joint_whole = jnp.concatenate([w for d in order for w in joint_pieces[d]], axis=0)
    both = jnp.dot(row_piece, joint_whole, preferred_element_type=jnp.float32)
    hidden = (jax.nn.silu(both[:, :part]) * both[:, part:]).astype(jnp.bfloat16)

    outs = []
    for chunk in (near, order[len(near) :]):
        if not chunk:
            continue
        down_whole = jnp.concatenate([w for d in chunk for w in down_pieces[d]], axis=0)
        partial = lax.dot_general(
            hidden, down_whole, (((1,), (1,)), ((), ())), preferred_element_type=jnp.float32
        ).astype(jnp.bfloat16)
        total = partial[:rows].astype(jnp.float32)
        for m, (dy, dt) in enumerate(members[1:], 1):
            got = group_move(partial[m * rows : (m + 1) * rows], dy, dt)
            total = total + got.astype(jnp.float32)
        outs.append(total.astype(jnp.bfloat16))
    mixed_out = jnp.concatenate(outs, axis=1)
    span = cores * pair * depth
    by_distance = jnp.concatenate(
        [lax.slice_in_dim(mixed_out, order.index(d) * span, (order.index(d) + 1) * span, axis=1)
         for d in range(chain)],
        axis=1,
    )
    pieces = []
    for a in range(chain):
        for b in range(pair):
            for c in range(cores):
                d, e = (a - z) % chain, (c - core) % cores
                at = ((d * cores + e) * pair + b) * depth
                pieces.append(lax.dynamic_slice_in_dim(by_distance, at, depth, axis=1))
    mixer_out = jnp.concatenate(pieces, axis=1)
    updated = middle.astype(jnp.float32) + 0.5 * mixer_out.astype(jnp.float32)
    return updated.astype(jnp.bfloat16)


def solution(mesh):
    return jax.shard_map(
        on_device,
        mesh=mesh,
        in_specs=(
            P(("grp", "sp", "tp"), None),
            P(("grp", "sp"), "tp"),
            P(("grp", "sp"), "tp"),
            P(("grp", "sp"), "tp"),
            P(("grp", "sp")),
            P("tp"),
            P("tp", None),
            P(),
            P("sp", "tp"),
            P("sp", "tp"),
            P("sp", "tp"),
        ),
        out_specs=P(("grp", "sp", "tp"), None),
        check_vma=False,
    )
```
